1024 devices in a mesh: sp: 16 (over z), dp: 64 (over y, x, core).
Axes of the slice: x: 4, y: 8, z: 16, core: 2. Of those that a mesh axis runs over, the one named last changes fastest.
Arguments:
- queries: bfloat16 [64, 768, 6144], P('dp', None, 'sp'), may hold values from -64 to 64
- out_grad: bfloat16 [64, 768, 4096], P('dp', None, 'sp'), may hold values from -6 to 6
- latent: bfloat16 [64, 768, 512], P('dp'), may hold values from -6 to 6
- rope_key: bfloat16 [64, 768, 64], P('dp'), may hold values from -6 to 6
- kv_gain: float32 [512], replicated, may hold values from 0.1 to 1.9
- key_up: bfloat16 [512, 4096], P('dp', 'sp'), may hold values from -0.25 to 0.25
- value_up: bfloat16 [512, 4096], P('dp', 'sp'), may hold values from -0.25 to 0.25
Outputs:
- query_grad: bfloat16 [64, 768, 6144], P('dp', None, 'sp')
- latent_grad: bfloat16 [64, 768, 512], P('dp')
- rope_key_grad: bfloat16 [64, 768, 64], P('dp')
- key_up_grad: float32 [512, 4096], P('dp', 'sp')
- value_up_grad: float32 [512, 4096], P('dp', 'sp')
The draws below stay inside these ranges and needn't reach their ends.
All inputs are finite; a program needn't handle non-finite values.
Results may differ from the reference program's by a relative error of at most 0.019.
The reference program's roundings to bfloat16 on the way count: a program that leaves them out, or rounds other values in their place, can miss the bound.
Values may be sent and summed in bfloat16 or wider, within the bound.
A program may use at most 32 MiB of HBM per device.

```python
import jax
import jax.numpy as jnp
from jax import lax

HEADS = 32
NOPE_DIM = 128
ROPE_DIM = 64
VALUE_DIM = 128
LATENT = 512
SEQ_LEN = 768
BATCH = 64
TOKENS = 49152
N_SP = 16


def draw_queries(key, part):
    shape = (BATCH, SEQ_LEN, HEADS * (NOPE_DIM + ROPE_DIM))
    base_key = jax.random.fold_in(key, 0)
    entries = jnp.clip(jax.random.normal(base_key, shape, jnp.float32), -6.0, 6.0)
    return entries.astype(jnp.bfloat16)


def shard_levels(stream_key, dims, pieces, smallest, high):
    level, own = 1.0, jax.random.fold_in(stream_key, 6)
    for dim, blocks in pieces:
        steps = jnp.exp(jax.random.uniform(jax.random.fold_in(own, dim), (blocks,), jnp.float32, smallest / len(pieces), high / len(pieces)))
        level = level * jnp.repeat(steps, dims[dim] // blocks).reshape([-1 if axis == dim else 1 for axis in range(len(dims))])
    return level


def normal_values(own_key, extent, scale, limit, shards=(), kind=jnp.bfloat16):
    result = jax.random.normal(own_key, extent, jnp.float32) * scale
    if len(shards) > 0:
        result = shard_levels(own_key, extent, shards, -0.22, 0.18) * result
    return jnp.clip(result, min=-limit, max=limit).astype(kind)


def setup_inputs(seed: int = 0) -> dict:
    splits = jax.random.split(jax.random.key(seed), 8)
    queries = draw_queries(jax.random.fold_in(splits[7], 71), 0)
    out_grad = normal_values(splits[1], (BATCH, SEQ_LEN, HEADS * VALUE_DIM), 1.0, 6.0, ((0, 64), (2, 16)))
    latent = normal_values(splits[2], (BATCH, SEQ_LEN, LATENT), 1.0, 6.0, ((0, 64),))
    rope_key = normal_values(splits[3], (BATCH, SEQ_LEN, ROPE_DIM), 1.0, 6.0, ((0, 64),))
    kv_gain = jnp.clip(1.0 + 0.18 * jax.random.normal(splits[4], (LATENT,), jnp.float32), 0.1, 1.9)
    key_up = normal_values(splits[5], (LATENT, HEADS * NOPE_DIM), LATENT ** -0.5, 0.25, ((0, 64), (1, 16)))
    value_up = normal_values(splits[6], (LATENT, HEADS * VALUE_DIM), LATENT ** -0.5, 0.25, ((0, 64), (1, 16)))
    return {"queries": queries, "out_grad": out_grad, "latent": latent, "rope_key": rope_key, "kv_gain": kv_gain, "key_up": key_up, "value_up": value_up}


norm_eps = 1e-06
rope_theta = 10000.0

def rope_tables(length, width):
    half_width = width // 2
    frequency = rope_theta ** (-(jnp.arange(half_width, dtype=jnp.float32) * 2.0 / width))
    position = jnp.arange(length, dtype=jnp.int32).astype(jnp.float32)
    angles = position[:, None] * frequency[None, :]
    return (jnp.cos(angles), jnp.sin(angles))

def rotate(tensor, cosine, sine_table):
    half_width = tensor.shape[-1] // 2
    first_half = tensor[..., :half_width]
    second = tensor[..., half_width:]
    return jnp.concatenate([first_half * cosine - second * sine_table, second * cosine + first_half * sine_table], axis=-1)

def unrotate(upstream, cosine, sine_table):
    half_width = upstream.shape[-1] // 2
    first_half = upstream[..., :half_width]
    second = upstream[..., half_width:]
    return jnp.concatenate([first_half * cosine + second * sine_table, second * cosine - first_half * sine_table], axis=-1)

def head_backward(query_used, key_used, head_value, head_grad, score_scale):
    length = query_used.shape[0]
    scores = jnp.dot(query_used, key_used.T, preferred_element_type=jnp.float32) * score_scale
    causal = lax.broadcasted_iota(jnp.int32, (length, length), 0) >= lax.broadcasted_iota(jnp.int32, (length, length), 1)
    scores = jnp.where(causal, scores, -jnp.inf)
    row_top = lax.optimization_barrier(jnp.max(scores, axis=1, keepdims=True))
    weights = jnp.exp(scores - row_top)
    probs = weights / lax.optimization_barrier(jnp.sum(weights, axis=1, keepdims=True))
    probs_low = probs.astype(jnp.bfloat16)
    value_grad = jnp.dot(probs_low.T, head_grad, preferred_element_type=jnp.float32).astype(jnp.bfloat16)
    prob_grad = jnp.dot(head_grad, head_value.T, preferred_element_type=jnp.float32)
    center = lax.optimization_barrier(jnp.sum(probs * prob_grad, axis=1, keepdims=True))
    score_grad = (probs * (prob_grad - center) * score_scale).astype(jnp.bfloat16)
    query_grad = jnp.dot(score_grad, key_used, preferred_element_type=jnp.float32)
    key_grad = jnp.dot(score_grad.T, query_used, preferred_element_type=jnp.float32)
    return (query_grad, key_grad, value_grad)

def attend(queries, head_grads, keys, values, key_rot, cosine, sine_table):
    length = queries.shape[0]
    head_count = head_grads.shape[1] // VALUE_DIM
    qk_width = NOPE_DIM + ROPE_DIM
    query_heads = queries.reshape(length, head_count, qk_width)
    rotated = rotate(query_heads[:, :, NOPE_DIM:].astype(jnp.float32), cosine[:, None, :], sine_table[:, None, :]).astype(jnp.bfloat16)
    query_used = jnp.concatenate([query_heads[:, :, :NOPE_DIM], rotated], axis=-1).transpose(1, 0, 2)
    key_heads = keys.reshape(length, head_count, NOPE_DIM).transpose(1, 0, 2)
    key_used = jnp.concatenate([key_heads, jnp.broadcast_to(key_rot[None], (head_count, length, ROPE_DIM))], axis=-1)
    value_heads = values.reshape(length, head_count, VALUE_DIM).transpose(1, 0, 2)
    grad_heads = head_grads.reshape(length, head_count, VALUE_DIM).transpose(1, 0, 2)
    score_scale = qk_width ** (-0.5)
    query_part, key_part, value_part = lax.map(lambda items: head_backward(items[0], items[1], items[2], items[3], score_scale), (query_used, key_used, value_heads, grad_heads))
    query_rot_grad = unrotate(query_part[:, :, NOPE_DIM:], cosine[None], sine_table[None])
    query_grad = jnp.concatenate([query_part[:, :, :NOPE_DIM], query_rot_grad], axis=-1).astype(jnp.bfloat16)
    query_grad = query_grad.transpose(1, 0, 2).reshape(length, head_count * qk_width)
    key_plain_grad = key_part[:, :, :NOPE_DIM].astype(jnp.bfloat16).transpose(1, 0, 2).reshape(length, head_count * NOPE_DIM)
    key_rot_grad = lax.optimization_barrier(jnp.sum(key_part[:, :, NOPE_DIM:], axis=0))
    value_grad = value_part.transpose(1, 0, 2).reshape(length, head_count * VALUE_DIM)
    return (query_grad, key_plain_grad, key_rot_grad, value_grad)

def finish(comp_total, rot_total, raw_latent, inverse, kv_gain, cosine, sine_table):
    mixed = comp_total * kv_gain
    spread = lax.optimization_barrier(jnp.mean(raw_latent * mixed, axis=-1, keepdims=True))
    latent_grad = (inverse * mixed - raw_latent * inverse ** 3 * spread).astype(jnp.bfloat16)
    rope_grad = unrotate(rot_total, cosine, sine_table).astype(jnp.bfloat16)
    return (latent_grad, rope_grad)

def reference(queries, out_grad, latent, rope_key, kv_gain, key_up, value_up):
    qk_width = NOPE_DIM + ROPE_DIM
    group = HEADS // N_SP
    cosine, sine_table = rope_tables(SEQ_LEN, ROPE_DIM)

    def one_sequence(totals, inputs):
        key_total, value_total = totals
        seq_queries, seq_grad, seq_latent, seq_rope = inputs
        raw_latent = seq_latent.astype(jnp.float32)
        inverse = lax.rsqrt(lax.optimization_barrier(jnp.mean(raw_latent * raw_latent, axis=-1, keepdims=True)) + norm_eps)
        compressed = (raw_latent * inverse * kv_gain).astype(jnp.bfloat16)
        key_rot = rotate(seq_rope.astype(jnp.float32), cosine, sine_table).astype(jnp.bfloat16)
        keys = jnp.dot(compressed, key_up, preferred_element_type=jnp.float32).astype(jnp.bfloat16)
        values = jnp.dot(compressed, value_up, preferred_element_type=jnp.float32).astype(jnp.bfloat16)

        def per_group(index):
            query_cols = lax.dynamic_slice_in_dim(seq_queries, index * (group * qk_width), group * qk_width, 1)
            grad_cols = lax.dynamic_slice_in_dim(seq_grad, index * (group * VALUE_DIM), group * VALUE_DIM, 1)
            key_cols = lax.dynamic_slice_in_dim(keys, index * (group * NOPE_DIM), group * NOPE_DIM, 1)
            value_cols = lax.dynamic_slice_in_dim(values, index * (group * VALUE_DIM), group * VALUE_DIM, 1)
            key_weight = lax.dynamic_slice_in_dim(key_up, index * (group * NOPE_DIM), group * NOPE_DIM, 1)
            value_weight = lax.dynamic_slice_in_dim(value_up, index * (group * VALUE_DIM), group * VALUE_DIM, 1)
            query_grad, key_plain_grad, key_rot_grad, value_grad = attend(query_cols, grad_cols, key_cols, value_cols, key_rot, cosine, sine_table)
            comp_part = jnp.dot(key_plain_grad, key_weight.T, preferred_element_type=jnp.float32) + jnp.dot(value_grad, value_weight.T, preferred_element_type=jnp.float32)
            return (query_grad, key_plain_grad, value_grad, comp_part, key_rot_grad)
        query_groups, key_groups, value_groups, comp_parts, rot_parts = lax.map(per_group, jnp.arange(N_SP, dtype=jnp.int32))
        query_grad = query_groups.transpose(1, 0, 2).reshape(SEQ_LEN, HEADS * qk_width)
        key_plain_all = key_groups.transpose(1, 0, 2).reshape(SEQ_LEN, HEADS * NOPE_DIM)
        value_all = value_groups.transpose(1, 0, 2).reshape(SEQ_LEN, HEADS * VALUE_DIM)
        comp_low = lax.optimization_barrier(comp_parts.astype(jnp.bfloat16))
        rot_low = lax.optimization_barrier(rot_parts.astype(jnp.bfloat16))
        comp_total = lax.optimization_barrier(jnp.sum(comp_low.astype(jnp.float32), axis=0))
        rot_total = lax.optimization_barrier(jnp.sum(rot_low.astype(jnp.float32), axis=0))
        latent_grad, rope_grad = finish(comp_total, rot_total, raw_latent, inverse, kv_gain, cosine, sine_table)
        contract = (((0,), (0,)), ((), ()))
        key_total = key_total + lax.dot_general(compressed, key_plain_all, contract, preferred_element_type=jnp.float32)
        value_total = value_total + lax.dot_general(compressed, value_all, contract, preferred_element_type=jnp.float32)
        return ((key_total, value_total), (query_grad, latent_grad, rope_grad))
    start_totals = (jnp.zeros((LATENT, HEADS * NOPE_DIM), jnp.float32), jnp.zeros((LATENT, HEADS * VALUE_DIM), jnp.float32))
    totals, outputs = lax.scan(one_sequence, start_totals, (queries, out_grad, latent, rope_key))
    grad_scale = float(TOKENS) ** (-0.5)
    return (outputs[0], outputs[1], outputs[2], totals[0] * grad_scale, totals[1] * grad_scale)
```

```python
import jax
import jax.numpy as jnp
import numpy as np
from jax import lax
from jax.experimental import pallas as pl
from jax.experimental.pallas import tpu as pltpu
from jax.sharding import PartitionSpec as P

MESH = pl.DeviceIdType.MESH
F32 = jnp.float32
BF16 = jnp.bfloat16

NX, NY, NC, NZ = 4, 8, 2, 16
SEQ = 768
LAT = 512
BLK = 256
NB = SEQ // BLK
HEADS = 2
SUB = BLK // NZ
WID = 640
NORM_EPS = 1e-06
SCORE_SCALE = 192 ** (-0.5)
LOG2E = 1.4426950408889634
GRAD_SCALE = 49152.0 ** (-0.5)


def rope_tables():
    steps = np.arange(32, dtype=np.float32) * np.float32(2.0) / np.float32(64)
    frequency = np.power(np.float32(10000.0), -steps).astype(np.float32)
    position = np.arange(SEQ, dtype=np.float32)
    angles = (position[:, None] * frequency[None, :]).astype(np.float32).astype(np.float64)
    cosine = np.cos(angles).astype(np.float32)
    sine = np.sin(angles).astype(np.float32)
    return (
        np.concatenate([cosine] * 4, axis=1),
        np.concatenate([-sine, sine, -sine, sine], axis=1),
    )


def lanes(shape):
    return lax.broadcasted_iota(jnp.int32, shape, len(shape) - 1)


def partner(t):
    lane = lanes(t.shape)
    axis = len(t.shape) - 1
    return jnp.where((lane % 64) < 32, pltpu.roll(t, 96, axis), pltpu.roll(t, 32, axis))


def turn(t, cosine, sine):
    return t * cosine + partner(t) * sine


def unturn(t, cosine, sine):
    return t * cosine - partner(t) * sine


def dot(a, b, dims):
    return lax.dot_general(a, b, (dims, ((), ())), preferred_element_type=F32)


NT = ((1,), (1,))
NN = ((1,), (0,))
TN = ((0,), (0,))


def kernel(
    q_ref, do_ref, lat_ref, rk_ref, gain_ref, ku_ref, vu_ref, cos_ref, sin_ref,
    qg_ref, lg_ref, rg_ref, kg_ref, vg_ref,
    gbuf, wk, wv, comp, q2, k2, v2, dk, dv, kpl, vgr,
    part, sb_r, rb_r, sb_l, rb_l, outb,
    gs, rc, hs, rx, ys, ry,
    sy, ry_sem, sx, rx_sem, sc, rc_sem,
    s_r, r_r, s_l, r_l, as_r, ar_r, as_l, ar_l,
    gsc, grc, gsx, grx, gsy, gry,
):
    z = lax.axis_index("sp")
    me = lax.axis_index("dp")
    c = lax.rem(me, NC)
    x = lax.rem(me // NC, NX)
    y = me // (NC * NX)

    def at(yy, xx, cc):
        return (z, (yy * NX + xx) * NC + cc)

    right = (lax.rem(z + 1, NZ), me)
    left = (lax.rem(z + NZ - 1, NZ), me)

    def other_y(k):
        return lax.rem(y + k, NY)

    def other_x(k):
        return lax.rem(x + k, NX)

    def remote(src, dst, send, recv, dev):
        return pltpu.make_async_remote_copy(
            src_ref=src, dst_ref=dst, send_sem=send, recv_sem=recv,
            device_id=dev, device_id_type=MESH,
        )

    barrier = pltpu.get_barrier_semaphore()
    for k in range(1, NY):
        pl.semaphore_signal(barrier, inc=1, device_id=at(other_y(k), x, c), device_id_type=MESH)
    for k in range(1, NX):
        pl.semaphore_signal(barrier, inc=1, device_id=at(y, other_x(k), c), device_id_type=MESH)
    pl.semaphore_signal(barrier, inc=1, device_id=at(y, x, 1 - c), device_id_type=MESH)
    pl.semaphore_signal(barrier, inc=1, device_id=right, device_id_type=MESH)
    pl.semaphore_signal(barrier, inc=1, device_id=left, device_id_type=MESH)
    pl.semaphore_wait(barrier, NY - 1 + NX - 1 + 3)

    gbuf[c, x, y] = jnp.concatenate(
        [ku_ref[...].astype(F32), vu_ref[...].astype(F32)], axis=0
    ).astype(BF16)

    def wcopy_y(k):
        return remote(gbuf.at[c, x, y], gbuf.at[c, x, y], sy.at[k], ry_sem.at[k], at(other_y(k), x, c))

    def wcopy_x(k):
        return remote(gbuf.at[c, x], gbuf.at[c, x], sx.at[k], rx_sem.at[k], at(y, other_x(k), c))

    def wcopy_c(k):
        xx = other_x(k)
        return remote(gbuf.at[c, xx], gbuf.at[c, xx], sc.at[k], rc_sem.at[k], at(y, x, 1 - c))

    for k in range(1, NY):
        wcopy_y(k).start()

    raw = lat_ref[...].astype(F32)
    inverse = lax.rsqrt(jnp.mean(raw * raw, axis=-1, keepdims=True) + NORM_EPS)
    comp[...] = (raw * inverse * gain_ref[...]).astype(BF16)
    cosine, sine = cos_ref[...], sin_ref[...]
    lane = lanes((SEQ, 128))
    low = lane < 64
    t1 = q_ref[:, 128:256].astype(F32)
    t1 = jnp.where(low, turn(t1, cosine, sine), t1).astype(BF16)
    t2 = q_ref[:, 256:384].astype(F32)
    t2 = jnp.where(low, t2, turn(t2, cosine, sine)).astype(BF16)
    q2[0, :, :128] = q_ref[:, :128]
    q2[0, :, 128:] = t1
    q2[1, :, :128] = t1
    q2[1, :, 128:] = t2
    key = rk_ref[...].astype(F32)
    key = turn(jnp.concatenate([key, key], axis=1), cosine, sine)
    k2[0, :, 128:] = jnp.where(low, key, 0.0).astype(BF16)

    for k in range(1, NY):
        wcopy_y(k).wait_recv()
    for k in range(1, NX):
        wcopy_x(k).start()
    wcopy_c(0).start()
    for k in (1, 3, 2):
        wcopy_x(k).wait_recv()
        wcopy_c(NX - k).start()
    for k in range(NX):
        wcopy_c(k).wait_recv()
    for k in range(1, NY):
        wcopy_y(k).wait_send()
    for k in range(1, NX):
        wcopy_x(k).wait_send()
    for k in range(NX):
        wcopy_c(k).wait_send()

    def place(i, _):
        g0 = gbuf[0, lax.rem(i, NX), i // NX].astype(F32)
        g1 = gbuf[1, lax.rem(i, NX), i // NX].astype(F32)
        rows = pl.ds(pl.multiple_of(i * 16, 16), 16)
        wk[rows, :] = jnp.concatenate([g0[:8], g1[:8]], axis=0).astype(BF16)
        wv[rows, :] = jnp.concatenate([g0[8:], g1[8:]], axis=0).astype(BF16)
        return 0

    lax.fori_loop(0, NX * NY, place, 0)

    keys = dot(comp[...], wk[...], NN)
    k2[0, :, :128] = keys[:, :128].astype(BF16)
    shifted = pltpu.roll(keys[:, 128:], 64, 1)
    k2[1, :, :128] = jnp.where(low, 0.0, shifted).astype(BF16)
    k2[1, :, 128:] = jnp.where(low, shifted, key).astype(BF16)
    v2[...] = dot(comp[...], wv[...], NN).astype(BF16)

    def first_r(j):
        return remote(part.at[j, lax.rem(z + 8, NZ)], rb_r.at[0, j], s_r.at[0, j], r_r.at[0, j], right)

    def first_l(j):
        return remote(part.at[j, lax.rem(z + NZ - 7, NZ)], rb_l.at[0, j], s_l.at[0, j], r_l.at[0, j], left)

    def next_r(s, j):
        return remote(sb_r.at[s, j], rb_r.at[s, j], s_r.at[s, j], r_r.at[s, j], right)

    def next_l(s, j):
        return remote(sb_l.at[s, j], rb_l.at[s, j], s_l.at[s, j], r_l.at[s, j], left)

    for i in reversed(range(NB)):
        n = (i + 1) * BLK
        rows = slice(i * BLK, n)
        qgs = []
        for h in range(HEADS):
            qi = q2[h, rows, :]
            doi = do_ref[rows, h * 128 : (h + 1) * 128]
            scores = dot(k2[h, :n, :], qi, NT)
            kpos = lax.broadcasted_iota(jnp.int32, (n, BLK), 0)
            qpos = lax.broadcasted_iota(jnp.int32, (n, BLK), 1) + i * BLK
            scores = jnp.where(kpos <= qpos, scores, -jnp.inf)
            top = jnp.max(scores, axis=0, keepdims=True)
            weights = jnp.exp2((scores - top) * (SCORE_SCALE * LOG2E))
            probs = weights * (1.0 / jnp.sum(weights, axis=0, keepdims=True))
            pgrad = dot(v2[:n, h * 128 : (h + 1) * 128], doi, NT)
            center = jnp.sum(probs * pgrad, axis=0, keepdims=True)
            sgrad = (probs * (pgrad - center) * SCORE_SCALE).astype(BF16)
            dvi = dot(probs.astype(BF16), doi, NN)
            dki = dot(sgrad, qi, NN)
            if i == NB - 1:
                dv[h] = dvi
                dk[h] = dki
            else:
                dv[h, :n, :] += dvi
                dk[h, :n, :] += dki
            qgs.append(dot(sgrad, k2[h, :n, :], TN))
        lowb = lanes((BLK, 128)) < 64
        cb, sbk = cos_ref[rows, :], sin_ref[rows, :]
        qg_ref[rows, :128] = qgs[0][:, :128].astype(BF16)
        g1 = qgs[0][:, 128:] + qgs[1][:, :128]
        qg_ref[rows, 128:256] = jnp.where(lowb, unturn(g1, cb, sbk), g1).astype(BF16)
        g2 = qgs[1][:, 128:]
        qg_ref[rows, 256:] = jnp.where(lowb, g2, unturn(g2, cb, sbk)).astype(BF16)

        ka, kb = dk[0, rows, :128], dk[0, rows, 128:]
        la, lb = dk[1, rows, :128], dk[1, rows, 128:]
        kp1 = pltpu.roll(jnp.where(lowb, lb, la), 64, 1)
        kp = jnp.concatenate([ka, kp1], axis=1).astype(BF16)
        vb = jnp.concatenate([dv[0, rows, :], dv[1, rows, :]], axis=1).astype(BF16)
        kpl[rows, :] = kp
        vgr[rows, :] = vb
        rot = jnp.where(lowb, kb + pltpu.roll(lb, 64, 1), 0.0)
        lat = dot(kp, wk[...], NT) + dot(vb, wv[...], NT)
        part[i, :, :, :LAT] = lat.astype(BF16).reshape(NZ, SUB, LAT)
        part[i, :, :, LAT:] = rot.astype(BF16).reshape(NZ, SUB, 128)
        first_r(i).start()
        first_l(i).start()

    pk = dot(comp[...], kpl[...], TN).reshape(NX * NY, 2, 8, 256)
    pv = dot(comp[...], vgr[...], TN).reshape(NX * NY, 2, 8, 256)
    for cc in range(NC):
        both = jnp.concatenate([pk[:, cc], pv[:, cc]], axis=1).astype(BF16)
        for yy in range(NY):
            for xx in range(NX):
                gs[cc, xx, yy] = both[yy * NX + xx]
    gcore = remote(gs.at[1 - c], rc, gsc, grc, at(y, x, 1 - c))
    gcore.start()

    def hop_r(s, j):
        next_owner = lax.rem(z + 7 - s, NZ)
        next_r(s, j).wait_recv()
        sb_r[s + 1, j] = (rb_r[s, j].astype(F32) + part[j, next_owner].astype(F32)).astype(BF16)
        next_r(s + 1, j).start()

    def hop_l(s, j):
        next_owner = lax.rem(z + NZ - 6 + s, NZ)
        next_l(s, j).wait_recv()
        sb_l[s + 1, j] = (rb_l[s, j].astype(F32) + part[j, next_owner].astype(F32)).astype(BF16)
        next_l(s + 1, j).start()

    order = tuple(reversed(range(NB)))

    def hops(s, _):
        for j in order:
            hop_r(s, j)
            hop_l(s, j)
        return 0

    lax.fori_loop(0, 1, hops, 0)

    gcore.wait_recv()
    for xx in range(NX):
        hs[xx] = (gs[c, xx].astype(F32) + rc[xx].astype(F32)).astype(BF16)

    def gcopy_x(k):
        return remote(hs.at[other_x(k)], rx.at[k], gsx.at[k], grx.at[k], at(y, other_x(k), c))

    for k in range(1, NX):
        gcopy_x(k).start()

    lax.fori_loop(1, 4, hops, 0)

    total = hs[x].astype(F32)
    for k in range(1, NX):
        gcopy_x(k).wait_recv()
        total += rx[k].astype(F32)
    ys[...] = total.astype(BF16)

    def gcopy_y(k):
        return remote(ys.at[other_y(k)], ry.at[k], gsy.at[k], gry.at[k], at(other_y(k), x, c))

    for k in range(1, NY):
        gcopy_y(k).start()

    lax.fori_loop(4, 6, hops, 0)
    for j in order:
        hop_r(6, j)

    def ag_r(s, j):
        o = lax.rem(z + NZ - s, NZ)
        return remote(outb.at[j, o], outb.at[j, o], as_r.at[s, j], ar_r.at[s, j], right)

    def ag_l(s, j):
        o = lax.rem(z + s, NZ)
        return remote(outb.at[j, o], outb.at[j, o], as_l.at[s, j], ar_l.at[s, j], left)

    for j in order:
        next_l(6, j).wait_recv()
        next_r(7, j).wait_recv()
        own = part[j, z].astype(F32) + rb_r[7, j].astype(F32) + rb_l[6, j].astype(F32)
        at_rows = pl.ds(pl.multiple_of(j * BLK + z * SUB, SUB), SUB)
        rw = lat_ref[at_rows, :].astype(F32)
        inv = lax.rsqrt(jnp.mean(rw * rw, axis=-1, keepdims=True) + NORM_EPS)
        u = own[:, :LAT] * gain_ref[...]
        spread = jnp.mean(rw * u, axis=-1, keepdims=True)
        outb[j, z, :, :LAT] = (inv * u - rw * (inv * inv * inv) * spread).astype(BF16)
        outb[j, z, :, LAT:] = unturn(own[:, LAT:], cos_ref[at_rows, :], sin_ref[at_rows, :]).astype(BF16)
        ag_r(0, j).start()
        ag_l(0, j).start()

    acc = ys[y].astype(F32)
    for k in range(1, NY):
        gcopy_y(k).wait_recv()
        acc += ry[k].astype(F32)
    acc = acc * GRAD_SCALE
    kg_ref[...] = acc[:8]
    vg_ref[...] = acc[8:]

    def relay(s, _):
        for j in order:
            ag_r(s, j).wait_recv()
            ag_r(s + 1, j).start()
            ag_l(s, j).wait_recv()
            ag_l(s + 1, j).start()
        return 0

    lax.fori_loop(0, 6, relay, 0)
    for j in order:
        ag_r(6, j).wait_recv()
        ag_r(7, j).start()
        ag_l(6, j).wait_recv()
    for j in order:
        ag_r(7, j).wait_recv()

    for j in range(NB):
        block = outb[j]
        lg_ref[j * BLK : (j + 1) * BLK, :] = block[:, :, :LAT].reshape(BLK, LAT)
        rg_ref[j * BLK : (j + 1) * BLK, :] = block[:, :, LAT : LAT + 64].reshape(BLK, 64)

    gcore.wait_send()
    for k in range(1, NX):
        gcopy_x(k).wait_send()
    for k in range(1, NY):
        gcopy_y(k).wait_send()
    for j in range(NB):
        first_r(j).wait_send()
        first_l(j).wait_send()

    def sent_r(s, _):
        for j in range(NB):
            next_r(s, j).wait_send()
        return 0

    def sent_l(s, _):
        for j in range(NB):
            next_l(s, j).wait_send()
        return 0

    def asent_r(s, _):
        for j in range(NB):
            ag_r(s, j).wait_send()
        return 0

    def asent_l(s, _):
        for j in range(NB):
            ag_l(s, j).wait_send()
        return 0

    lax.fori_loop(1, 8, sent_r, 0)
    lax.fori_loop(1, 7, sent_l, 0)
    lax.fori_loop(0, 8, asent_r, 0)
    lax.fori_loop(0, 7, asent_l, 0)


def shards(queries, out_grad, latent, rope_key, kv_gain, key_up, value_up):
    cosine, sine = rope_tables()
    vmem = pl.BlockSpec(memory_space=pltpu.VMEM)
    dma = pltpu.SemaphoreType.DMA
    outs = pl.pallas_call(
        kernel,
        out_shape=(
            jax.ShapeDtypeStruct((SEQ, 384), BF16),
            jax.ShapeDtypeStruct((SEQ, LAT), BF16),
            jax.ShapeDtypeStruct((SEQ, 64), BF16),
            jax.ShapeDtypeStruct((8, 256), F32),
            jax.ShapeDtypeStruct((8, 256), F32),
        ),
        in_specs=[vmem] * 9,
        out_specs=(vmem,) * 5,
        scratch_shapes=[
            pltpu.VMEM((NC, NX, NY, 16, 256), BF16),
            pltpu.VMEM((LAT, 256), BF16),
            pltpu.VMEM((LAT, 256), BF16),
            pltpu.VMEM((SEQ, LAT), BF16),
            pltpu.VMEM((HEADS, SEQ, 256), BF16),
            pltpu.VMEM((HEADS, SEQ, 256), BF16),
            pltpu.VMEM((SEQ, 256), BF16),
            pltpu.VMEM((HEADS, SEQ, 256), F32),
            pltpu.VMEM((HEADS, SEQ, 128), F32),
            pltpu.VMEM((SEQ, 256), BF16),
            pltpu.VMEM((SEQ, 256), BF16),
            pltpu.VMEM((NB, NZ, SUB, WID), BF16),
            pltpu.VMEM((8, NB, SUB, WID), BF16),
            pltpu.VMEM((8, NB, SUB, WID), BF16),
            pltpu.VMEM((7, NB, SUB, WID), BF16),
            pltpu.VMEM((7, NB, SUB, WID), BF16),
            pltpu.VMEM((NB, NZ, SUB, WID), BF16),
            pltpu.VMEM((NC, NX, NY, 16, 256), BF16),
            pltpu.VMEM((NX, NY, 16, 256), BF16),
            pltpu.VMEM((NX, NY, 16, 256), BF16),
            pltpu.VMEM((NX, NY, 16, 256), BF16),
            pltpu.VMEM((NY, 16, 256), BF16),
            pltpu.VMEM((NY, 16, 256), BF16),
            dma((NY,)), dma((NY,)), dma((NX,)), dma((NX,)), dma((NX,)), dma((NX,)),
            dma((8, NB)), dma((8, NB)), dma((7, NB)), dma((7, NB)),
            dma((8, NB)), dma((8, NB)), dma((7, NB)), dma((7, NB)),
            dma, dma, dma((NX,)), dma((NX,)), dma((NY,)), dma((NY,)),
        ],
        compiler_params=pltpu.CompilerParams(collective_id=0, has_side_effects=True),
    )(
        queries[0], out_grad[0], latent[0], rope_key[0], kv_gain[None], key_up, value_up,
        jnp.asarray(cosine), jnp.asarray(sine),
    )
    query_grad, latent_grad, rope_grad, key_grad, value_grad = outs
    return (query_grad[None], latent_grad[None], rope_grad[None], key_grad, value_grad)


def solution(mesh):
    return jax.shard_map(
        shards,
        mesh=mesh,
        in_specs=(
            P("dp", None, "sp"),
            P("dp", None, "sp"),
            P("dp", None, None),
            P("dp", None, None),
            P(),
            P("dp", "sp"),
            P("dp", "sp"),
        ),
        out_specs=(
            P("dp", None, "sp"),
            P("dp", None, None),
            P("dp", None, None),
            P("dp", "sp"),
            P("dp", "sp"),
        ),
        check_vma=False,
    )
```
